32 devices in a mesh: tp: 8 (over z, y), dp: 4 (over x, core).
Axes of the slice: x: 2, y: 2, z: 4, core: 2. Of those that a mesh axis runs over, the one named last changes fastest.
Arguments:
- activation_rows: bfloat16 [1024, 4096], P(None, 'dp'), may hold values from -24 to 24
- fresh_spans: int32 [128], P('dp'), may hold values from 1 to 8, 384 in all
- entry_rescale_vector: float32 [2, 4096], P(None, 'dp'), may hold values from 0.1 to 1.9
- probe_kernel: bfloat16 [2, 4096, 4096], P(None, 'dp', 'tp'), may hold values from -0.09375 to 0.09375
- retention_kernel: bfloat16 [2, 4096, 4096], P(None, 'dp', 'tp'), may hold values from -0.09375 to 0.09375
- content_kernel: bfloat16 [2, 4096, 4096], P(None, 'dp', 'tp'), may hold values from -0.09375 to 0.09375
- valve_kernel: bfloat16 [2, 4096, 4096], P(None, 'dp', 'tp'), may hold values from -0.09375 to 0.09375
- retention_minimum: float32 [2, 4096], P(None, 'tp'), may hold values from 0 to 0.99
- extra_attenuation: float32 [2, 1024, 32], P(None, 'dp', 'tp'), may hold values from -0.7 to 0
- channel_rescale_vector: float32 [2, 4096], P(None, 'tp'), may hold values from 0.1 to 1.9
- emission_kernel: bfloat16 [2, 4096, 4096], P(None, 'tp', 'dp'), may hold values from -0.09375 to 0.09375
- memory_grids: float32 [2, 128, 32, 128, 128], P(None, 'dp', 'tp'), may hold values from -0.6 to 0.6
Outputs:
- mixed: bfloat16 [1024, 4096], P(None, 'dp')
- new_states: float32 [2, 128, 32, 128, 128], P(None, 'dp', 'tp')
The draws below stay inside these ranges and needn't reach their ends.
Inputs may be any that keep to these rules, and one draw needn't show every extreme that they name: `fresh_spans`: each sequence has at least one live slot.
All inputs are finite; a program needn't handle non-finite values. No bound on the sum of `fresh_spans` on one device may be relied on, other than what follows from the above.
Results may differ from the reference program's by a relative error of at most 0.017.
Values may be sent and summed in bfloat16 or wider, within the bound.
A program may use at most 128 MiB of HBM per device.

```python
import math
import jax
import jax.numpy as jnp
import numpy as np
from jax import lax

D = 4096
HEADS = 32
DK = 128
DV = 128
NEW = 8
BLOCKS = 2
SEQS = 128
ROWS = 1024
HK = 4096
HV = 4096
N_DP = 4


def draw_activation_rows(key, part):
    column_scale = jnp.exp(jnp.linspace(0.0, math.log(4.0), D, dtype=jnp.float32))[None, :]
    base = jnp.clip(jax.random.normal(key, (ROWS, D), jnp.float32), -6.0, 6.0)
    return jnp.clip(base * column_scale, -24.0, 24.0).astype(jnp.bfloat16)


def draw_extra_attenuation(key, part):
    hits = jax.random.randint(jax.random.fold_in(key, 3), (BLOCKS, ROWS, HEADS), 0, 10) == 0
    depth = jax.random.uniform(jax.random.fold_in(key, 4), (BLOCKS, ROWS, HEADS), jnp.float32, math.log(0.5), math.log(0.8))
    return jnp.where(hits, depth, jnp.zeros_like(depth)).astype(jnp.float32)


def levels(stream_key, dims, cuts, smallest, high):
    factor_of = 1.0
    for position, parts in cuts:
        heights = jax.random.uniform(jax.random.fold_in(jax.random.fold_in(stream_key, 6), position), (parts,), jnp.float32, smallest / len(cuts), high / len(cuts))
        factor_of = factor_of * jnp.repeat(jnp.exp(heights), dims[position] // parts).reshape((-1,) + (1,) * (len(dims) - 1 - position))
    return factor_of


def length_profile(count, total, most, skew):
    loads = [(1 << 20) // math.isqrt(standing ** skew) + 1 for standing in range(2, count + 1)]
    surplus, holding = total - most - (count - 1), [1] * (count - 1)
    while surplus > 0:
        candidates = [i for i in range(count - 1) if holding[i] < most]
        mass, left = sum([loads[i] for i in candidates]), surplus
        for i in candidates:
            more = min(most - holding[i], max(1, left * loads[i] // mass), surplus)
            holding[i] = holding[i] + more
            surplus = surplus - more
    return np.array([most] + holding)


def ragged(stream_key, count, total, reach, skew):
    if count == 2:
        one = jax.random.randint(stream_key, (), max(1, total - reach), min(reach, total - 1) + 1)
        return jnp.stack([one, total - one])
    tallies = jnp.asarray(length_profile(count, total, reach, skew), jnp.int32)
    twos = (count - 1) // 2
    giver, receiver = tallies[1:1 + 2 * twos:2], tallies[2:2 + 2 * twos:2]
    room = jnp.minimum(giver - 1, reach - receiver)
    passed = jax.random.randint(jax.random.fold_in(stream_key, 1), (twos,), 0, 1 << 20) % (room + 1)
    tallies = tallies.at[1:1 + 2 * twos:2].set(giver - passed).at[2:2 + 2 * twos:2].set(receiver + passed)
    return tallies[jax.random.permutation(jax.random.fold_in(stream_key, 2), count)]


def noise(rng, dims, scale, most, split=(), kind=jnp.bfloat16):
    result = jax.random.normal(rng, dims, jnp.float32) * scale
    if len(split) > 0:
        result = levels(rng, dims, split, -0.22, 0.18) * result
    return jnp.clip(result, min=-most, max=most).astype(kind)


def setup_inputs(seed: int = 0) -> dict:
    splits = jax.random.split(jax.random.key(seed), 13)
    return {
        "activation_rows": draw_activation_rows(jax.random.fold_in(splits[12], 71), 0),
        "fresh_spans": ragged(splits[1], SEQS, 3 * SEQS, NEW, 2).astype(jnp.int32),
        "entry_rescale_vector": jnp.clip(1.0 + 0.18 * jax.random.normal(splits[2], (BLOCKS, D), jnp.float32), 0.1, 1.9),
        "probe_kernel": noise(splits[3], (BLOCKS, D, HK), D ** -0.5, 0.09375, ((1, 4), (2, 8))),
        "retention_kernel": noise(splits[4], (BLOCKS, D, HK), D ** -0.5, 0.09375, ((1, 4), (2, 8))),
        "content_kernel": noise(splits[5], (BLOCKS, D, HV), D ** -0.5, 0.09375, ((1, 4), (2, 8))),
        "valve_kernel": noise(splits[6], (BLOCKS, D, HV), D ** -0.5, 0.09375, ((1, 4), (2, 8))),
        "retention_minimum": jnp.clip(0.99 * jax.random.uniform(splits[7], (BLOCKS, HK), jnp.float32) ** levels(splits[7], (BLOCKS, HK), ((1, 8),), -0.2, 0.2), 0.0, 0.99),
        "extra_attenuation": draw_extra_attenuation(jax.random.fold_in(splits[12], 71), 0),
        "channel_rescale_vector": jnp.clip(1.0 + 0.18 * jax.random.normal(splits[9], (BLOCKS, HV), jnp.float32), 0.1, 1.9),
        "emission_kernel": noise(splits[10], (BLOCKS, HV, D), HV ** -0.5, 0.09375, ((1, 8), (2, 4))),
        "memory_grids": noise(splits[11], (BLOCKS, SEQS, HEADS, DK, DV), 0.1, 0.6, ((1, 4), (2, 8)), jnp.float32),
    }


EPSILON = 1e-05

def update_tick(probe_scores, retention_scores, content_scores, valve_scores, minimum_bound, spike_ledger, attention_multiplier, stream_spans, memory_grid):
    stream_tally = memory_grid.shape[0]
    attention_tally = memory_grid.shape[1]
    key_dim = memory_grid.shape[2]
    value_dim = memory_grid.shape[3]
    position_tally = probe_scores.shape[0] // stream_tally

    def split_heads(array, width):
        return array.astype(jnp.float32).reshape(stream_tally, position_tally, attention_tally, width)
    queries = jax.nn.silu(split_heads(probe_scores, key_dim))
    forget_in = split_heads(retention_scores, key_dim)
    lower_heads = minimum_bound.reshape(attention_tally, key_dim)
    retention_sigmoid = lower_heads + (1.0 - lower_heads) * jax.nn.sigmoid(forget_in)
    key_vecs = (1.0 - lower_heads) * jax.nn.sigmoid(-forget_in)
    log_attenuation = jnp.log(retention_sigmoid) + spike_ledger.reshape(stream_tally, position_tally, attention_tally)[..., None]
    values = split_heads(content_scores, value_dim)
    positions = lax.broadcasted_iota(jnp.int32, (stream_tally, position_tally), 1)
    live_mask = positions < stream_spans[:, None].astype(jnp.int32)

    def advance(matrix, inputs):
        query_now, key_now, decay_now, value_now, live_now = inputs
        updated = jnp.exp(decay_now)[..., None] * matrix + key_now[..., None] * value_now[..., None, :]
        matrix = jnp.where(live_now[:, None, None, None], updated, matrix)
        readout = jnp.einsum('shkv,shk->shv', matrix, query_now, precision=lax.Precision.HIGHEST)
        return (matrix, readout)
    ending_emission, readouts = lax.scan(advance, memory_grid, (jnp.moveaxis(queries, 1, 0), jnp.moveaxis(key_vecs, 1, 0), jnp.moveaxis(log_attenuation, 1, 0), jnp.moveaxis(values, 1, 0), jnp.moveaxis(live_mask, 1, 0)))
    readouts = jnp.moveaxis(readouts, 0, 1)
    normed = readouts * lax.rsqrt(lax.optimization_barrier(jnp.mean(readouts * readouts, axis=-1, keepdims=True)) + EPSILON)
    normed = normed * attention_multiplier.reshape(attention_tally, value_dim) * jax.nn.silu(split_heads(valve_scores, value_dim))
    normed = normed * live_mask.astype(jnp.float32)[..., None, None]
    return (normed.reshape(stream_tally * position_tally, attention_tally * value_dim).astype(jnp.bfloat16), ending_emission)

def blocked_product(normed, weight):
    width = D // N_DP
    total = jnp.zeros((normed.shape[0], weight.shape[1]), jnp.float32)
    for index in range(N_DP):
        partial_value = jnp.dot(normed[:, index * width:(index + 1) * width], weight[index * width:(index + 1) * width], preferred_element_type=jnp.float32)
        rounded = lax.optimization_barrier(partial_value.astype(jnp.bfloat16))
        total = total + rounded.astype(jnp.float32)
    return total

def reference(activation_rows, fresh_spans, entry_rescale_vector, probe_kernel, retention_kernel, content_kernel, valve_kernel, retention_minimum, extra_attenuation, channel_rescale_vector, emission_kernel, memory_grids):
    residual = activation_rows
    finals = []
    for layer_index in range(BLOCKS):
        current = residual.astype(jnp.float32)
        row_scale = lax.rsqrt(lax.optimization_barrier(jnp.mean(current * current, axis=1)) + EPSILON)
        normed = (current * entry_rescale_vector[layer_index]).astype(jnp.bfloat16)
        mapped_activation = [(blocked_product(normed, weight[layer_index]) * row_scale[:, None]).astype(jnp.bfloat16) for weight in (probe_kernel, retention_kernel, content_kernel, valve_kernel)]
        attention_yields, ending_emission = update_tick(mapped_activation[0], mapped_activation[1], mapped_activation[2], mapped_activation[3], retention_minimum[layer_index], extra_attenuation[layer_index], channel_rescale_vector[layer_index], fresh_spans, memory_grids[layer_index])
        finals.append(ending_emission)
        update = jnp.dot(attention_yields, emission_kernel[layer_index], preferred_element_type=jnp.float32).astype(jnp.bfloat16)
        residual = (current + update.astype(jnp.float32)).astype(jnp.bfloat16)
    return (residual, jnp.stack(finals))
```

```python
import functools

import jax
import jax.numpy as jnp
from jax import lax
from jax.experimental import pallas as pl
from jax.experimental.pallas import tpu as pltpu
from jax.sharding import PartitionSpec as P

EPSILON = 1e-05
F32, BF16 = jnp.float32, jnp.bfloat16
MESH = pl.DeviceIdType.MESH
LIVE_PER_SEQUENCE = 3
GROUP = 8
VMEM_LIMIT = 62 * 1024 * 1024


def peer(axis, offset):
    size = lax.axis_size(axis)
    return lax.rem(lax.axis_index(axis) + offset, size)


def aligned(start):
    return pl.multiple_of(start, 16)


def comm_kernel(sizes, has_out, layer, *refs):
    n, t, rows, live, feats, chans = sizes
    refs = list(refs)
    take = lambda: refs.pop(0)
    posrow_ref = take()
    if has_out:
        ho_ref, xc_in, we_ref = take(), take(), take()
    else:
        x_ref = take()
    if layer is not None:
        poscol_ref, gain_ref = take(), take()
        w_refs = [take() for _ in range(4)]
        z_ref = take()
    xc_out = take()
    if has_out:
        we_buf, we_sem = take(), take()
        hg, h_send, h_recv = take(), take(), take()
        h_fsend, h_frecv, upart, ufull = take(), take(), take(), take()
        halves = [[take() for _ in range(11)] for _ in range(2)]
    if layer is not None:
        w_buf, w_sem = take(), take()
        nb, part, pair_recv, x_send, x_recv, full = (take() for _ in range(6))
        pair_s, pair_r, xs, xr, ag_s, ag_r, fw_s, fw_r = (take() for _ in range(8))
        ssq, ssq_recv, sq_s, sq_r = take(), take(), take(), take()
    me, mt = lax.axis_index("dp"), lax.axis_index("tp")
    own = rows // n
    chips = n // 2
    chip, core = me // 2, lax.rem(me, 2)
    partner = chip * 2 + 1 - core

    def beside(k):
        return lax.rem(chip + k, chips) * 2 + core

    if has_out:
        we_copy = pltpu.make_async_copy(we_ref.at[(layer - 1) if layer is not None else 1], we_buf, we_sem)
        we_copy.start()
    if layer is not None:
        w_copies = [
            pltpu.make_async_copy(w_refs[w].at[layer], w_buf.at[w], w_sem.at[w]) for w in range(4)
        ]
        for copy in w_copies:
            copy.start()
    barrier = pltpu.get_barrier_semaphore()
    for k in range(1, n):
        pl.semaphore_signal(barrier, inc=1, device_id={"dp": peer("dp", k)}, device_id_type=MESH)
    if has_out:
        for k in range(1, t):
            pl.semaphore_signal(
                barrier, inc=1, device_id={"tp": peer("tp", k)}, device_id_type=MESH
            )
    expected = n - 1 + (t - 1 if has_out else 0)
    pending = []

    def remote(src, dst, send, recv, axis, target):
        return pltpu.make_async_remote_copy(
            src_ref=src, dst_ref=dst, send_sem=send, recv_sem=recv,
            device_id={axis: target}, device_id_type=MESH,
        )

    step = 128
    if has_out:
        pl.semaphore_wait(barrier, expected)
        copies = []
        for k in range(chips):
            target = partner if k == 0 else beside(k)
            copy = remote(ho_ref, hg.at[me], h_send.at[k], h_recv.at[k], "dp", target)
            copy.start()
            copies.append(copy)
        hg[me] = ho_ref[...]
        forwards = []
        for k in range(1, chips):
            copies[k].wait_recv()
            source = beside(chips - k)
            copy = remote(
                hg.at[source], hg.at[source], h_fsend.at[k - 1], h_frecv.at[k - 1], "dp", partner
            )
            copy.start()
            forwards.append(copy)
        we_copy.wait()
        copies[0].wait_recv()
        for copy in forwards:
            copy.wait_recv()
        pending += copies + forwards
        gathered = hg[...].reshape(rows, chans)
        for i in range(live // step):
            pick = (
                lax.broadcasted_iota(jnp.int32, (step, rows), 0) + i * step == posrow_ref[...]
            ).astype(F32).astype(BF16)
            hc = jnp.dot(pick, gathered, preferred_element_type=F32).astype(BF16)
            upart[pl.ds(i * step, step), :] = jnp.dot(
                hc, we_buf[...], preferred_element_type=F32
            ).astype(BF16)
        deep = 4 if t % 4 == 0 else 1
        flat = t // deep
        iz, iy = mt // flat, lax.rem(mt, flat)
        along_y = (flat, iy, lambda j: iz * flat + j)
        along_z = (deep, iz, lambda j: j * flat + iy)
        plans = [(along_y, along_z), (along_z, along_y)]
        width = feats // 2
        fine = live // t

        def send(group, src, dst, send_sem, recv_sem, target):
            copy = remote(src, dst, send_sem, recv_sem, "tp", target)
            copy.start()
            group.append(copy)

        def start(half, stage):
            (s1, i1, to1), (s2, i2, to2) = plans[half]
            r1, t1, r2, *sems = halves[half]
            s_sem, r_sem = sems[2 * stage], sems[2 * stage + 1]
            cols = pl.ds(half * width, width)
            coarse = live // s1
            block = pl.ds(aligned(i1 * coarse), coarse)
            mine = pl.ds(aligned(i1 * coarse + i2 * fine), fine)
            size, index, to = ((s1, i1, to1), (s2, i2, to2))[stage in (1, 2)]
            group = []
            for k in range(1, size):
                j = lax.rem(index + k, size)
                if stage == 0:
                    src = upart.at[pl.ds(aligned(j * coarse), coarse), cols]
                    dst = r1.at[k - 1]
                elif stage == 1:
                    src, dst = t1.at[pl.ds(aligned(j * fine), fine)], r2.at[k - 1]
                else:
                    where = mine if stage == 2 else block
                    src = dst = ufull.at[where, cols]
                send(group, src, dst, s_sem.at[k - 1], r_sem.at[k - 1], to(j))
            return group

        def finish(half, stage, group):
            (s1, i1, _), (s2, i2, _) = plans[half]
            r1, t1, r2 = halves[half][:3]
            cols = pl.ds(half * width, width)
            coarse = live // s1
            for copy in group:
                copy.wait_recv()
            if stage == 0:
                total = upart[pl.ds(aligned(i1 * coarse), coarse), cols].astype(F32)
                for k in range(s1 - 1):
                    total = total + r1[k].astype(F32)
                t1[...] = total.astype(BF16)
            elif stage == 1:
                total = t1[pl.ds(aligned(i2 * fine), fine), :].astype(F32)
                for k in range(s2 - 1):
                    total = total + r2[k].astype(F32)
                mine = pl.ds(aligned(i1 * coarse + i2 * fine), fine)
                ufull[mine, cols] = total.astype(BF16)
            return group

        groups = [start(half, 0) for half in range(2)]
        for stage in range(4):
            for half in range(2):
                pending += finish(half, stage, groups[half])
                if stage < 3:
                    groups[half] = start(half, stage + 1)
    for i in range(live // step):
        span = pl.ds(i * step, step)
        if has_out:
            cur = (xc_in[span, :].astype(F32) + ufull[span, :].astype(F32)).astype(BF16)
        else:
            pick = (
                lax.broadcasted_iota(jnp.int32, (step, rows), 0) + i * step == posrow_ref[...]
            ).astype(F32).astype(BF16)
            cur = jnp.dot(pick, x_ref[...], preferred_element_type=F32).astype(BF16)
        xc_out[span, :] = cur
        if layer is not None:
            cur = cur.astype(F32)
            nb[span, :] = (cur * gain_ref[layer : layer + 1, :]).astype(BF16)
            squares = jnp.sum(cur * cur, axis=1, keepdims=True)
            hi = squares.astype(BF16).astype(F32)
            mid = (squares - hi).astype(BF16).astype(F32)
            low = squares - hi - mid
            lane = lax.broadcasted_iota(jnp.int32, (step, 128), 1)
            ssq[span, :] = jnp.where(
                lane == 0, hi, jnp.where(lane == 1, mid, jnp.where(lane == 2, low, 0.0))
            ).astype(BF16)
    if layer is not None:
        if not has_out:
            pl.semaphore_wait(barrier, expected)
        chunk = live // n
        mine = pl.ds(aligned(me * chunk), chunk)
        sq_copies = []
        for k in range(1, n):
            src = pl.ds(aligned(peer("dp", k) * chunk), chunk)
            copy = remote(
                ssq.at[src], ssq_recv.at[k - 1], sq_s.at[k - 1], sq_r.at[k - 1],
                "dp", peer("dp", k),
            )
            copy.start()
            sq_copies.append(copy)
        pairs, crossings = [], []

        def chunk_of(index, side):
            return pl.ds(aligned((index * 2 + side) * chunk), chunk)

        def cross(w):
            group = []
            for k in range(1, chips):
                pairs[w][k].wait_recv()
                rows_k = chunk_of(lax.rem(chip + k, chips), core)
                x_send[w, k - 1] = (
                    part[w, rows_k, :].astype(F32) + pair_recv[w, k].astype(F32)
                ).astype(BF16)
                copy = remote(
                    x_send.at[w, k - 1], x_recv.at[w, k - 1], xs.at[w, k - 1], xr.at[w, k - 1],
                    "dp", beside(k),
                )
                copy.start()
                group.append(copy)
            crossings.append(group)

        for w in range(4):
            w_copies[w].wait()
            part[w] = jnp.dot(nb[...], w_buf[w], preferred_element_type=F32).astype(BF16)
            group = []
            for k in range(chips):
                src = chunk_of(lax.rem(chip + k, chips), 1 - core)
                copy = remote(
                    part.at[w, src], pair_recv.at[w, k], pair_s.at[w, k], pair_r.at[w, k],
                    "dp", partner,
                )
                copy.start()
                group.append(copy)
            pairs.append(group)
            if w > 0:
                cross(w - 1)
        cross(3)
        squares = jnp.sum(ssq[mine, :].astype(F32), axis=1, keepdims=True)
        for k in range(1, n):
            sq_copies[k - 1].wait_recv()
            squares = squares + jnp.sum(ssq_recv[k - 1].astype(F32), axis=1, keepdims=True)
        scale = lax.rsqrt(squares / (feats * n) + EPSILON)
        ag = []
        for w in range(4):
            pairs[w][0].wait_recv()
            total = part[w, mine, :].astype(F32) + pair_recv[w, 0].astype(F32)
            for k in range(1, chips):
                crossings[w][k - 1].wait_recv()
                total = total + x_recv[w, k - 1].astype(F32)
            full[w, mine, :] = (total * scale).astype(BF16)
            group = []
            for k in [*range(1, chips), 0]:
                copy = remote(
                    full.at[w, mine], full.at[w, mine], ag_s.at[w, k], ag_r.at[w, k],
                    "dp", partner if k == 0 else beside(k),
                )
                copy.start()
                group.append(copy)
            ag.append(group)
        forwards = []
        for w in range(4):
            group = []
            for k in range(1, chips):
                ag[w][k - 1].wait_recv()
                block = chunk_of(lax.rem(chip + chips - k, chips), core)
                copy = remote(
                    full.at[w, block], full.at[w, block], fw_s.at[w, k - 1], fw_r.at[w, k - 1],
                    "dp", partner,
                )
                copy.start()
                group.append(copy)
            forwards.append(group)
        spread = (
            lax.broadcasted_iota(jnp.int32, (own, live), 1)
            == poscol_ref[pl.ds(aligned(me * own), own), :]
        ).astype(F32).astype(BF16)
        for w in range(4):
            ag[w][-1].wait_recv()
            for copy in forwards[w]:
                copy.wait_recv()
            z_ref[:, w * chans : (w + 1) * chans] = jnp.dot(
                spread, full[w], preferred_element_type=F32
            ).astype(BF16)
            pending += pairs[w] + crossings[w] + ag[w] + forwards[w]
        pending += sq_copies
    for copy in pending:
        copy.wait_send()


def comm_call(sizes, has_out, layer, collective_id, args):
    n, t, rows, live, feats, chans = sizes
    vmem, hbm = pl.BlockSpec(memory_space=pltpu.VMEM), pl.BlockSpec(memory_space=pl.ANY)
    dma = pltpu.SemaphoreType.DMA
    chips = n // 2
    in_specs = [vmem]
    in_specs += [vmem, vmem, hbm] if has_out else [vmem]
    out_shape, scratch = [], []
    if layer is not None:
        in_specs += [vmem, vmem] + [hbm] * 4
        out_shape.append(jax.ShapeDtypeStruct((rows // n, 4 * chans), BF16))
    out_shape.append(jax.ShapeDtypeStruct((live, feats), BF16))
    if has_out:
        scratch += [
            pltpu.VMEM((chans, feats), BF16), dma,
            pltpu.VMEM((n, rows // n, chans), BF16), dma((chips,)), dma((chips,)),
            dma((chips - 1,)), dma((chips - 1,)),
            pltpu.VMEM((live, feats), BF16),
            pltpu.VMEM((live, feats), BF16),
        ]
        deep = 4 if t % 4 == 0 else 1
        for s1, s2 in ((t // deep, deep), (deep, t // deep)):
            scratch += [
                pltpu.VMEM((s1 - 1, live // s1, feats // 2), BF16),
                pltpu.VMEM((live // s1, feats // 2), BF16),
                pltpu.VMEM((s2 - 1, live // t, feats // 2), BF16),
            ]
            for size in (s1, s2, s2, s1):
                scratch += [dma((size - 1,)), dma((size - 1,))]
    if layer is not None:
        chunk = live // n
        scratch += [
            pltpu.VMEM((4, feats, chans), BF16), dma((4,)),
            pltpu.VMEM((live, feats), BF16),
            pltpu.VMEM((4, live, chans), BF16),
            pltpu.VMEM((4, chips, chunk, chans), BF16),
            pltpu.VMEM((4, chips - 1, chunk, chans), BF16),
            pltpu.VMEM((4, chips - 1, chunk, chans), BF16),
            pltpu.VMEM((4, live, chans), BF16),
            dma((4, chips)), dma((4, chips)), dma((4, chips - 1)), dma((4, chips - 1)),
            dma((4, chips)), dma((4, chips)), dma((4, chips - 1)), dma((4, chips - 1)),
            pltpu.VMEM((live, 128), BF16),
            pltpu.VMEM((n - 1, chunk, 128), BF16),
            dma((n - 1,)), dma((n - 1,)),
        ]
    return pl.pallas_call(
        functools.partial(comm_kernel, sizes, has_out, layer),
        out_shape=out_shape,
        in_specs=in_specs,
        out_specs=[vmem] * len(out_shape),
        scratch_shapes=scratch,
        compiler_params=pltpu.CompilerParams(
            collective_id=collective_id, has_side_effects=True, vmem_limit_bytes=VMEM_LIMIT
        ),
        name=f"comm{collective_id}",
    )(*args)


def recurrence_kernel(layer, heads, new, z_ref, ext_ref, low_ref, gain_ref, s_ref, *rest):
    ho_ref, ns_ref = rest[-2:]
    group, width = s_ref.shape[1], s_ref.shape[3]
    chans = heads * width
    lines = group * new
    live = ext_ref[:, heads : heads + 1] > 0.5
    row = lax.broadcasted_iota(jnp.int32, (lines, width), 0)
    slot = lax.broadcasted_iota(jnp.int32, (group, new, width), 1)
    for h in range(heads):
        cols = slice(h * width, (h + 1) * width)

        def piece(w):
            start = w * chans + h * width
            return z_ref[:, start : start + width].astype(F32)

        query, forget, value, gate = (piece(w) for w in range(4))
        low = low_ref[layer : layer + 1, cols]
        query = query * jax.nn.sigmoid(query)
        decay = (low + (1.0 - low) * jax.nn.sigmoid(forget)) * jnp.exp(ext_ref[:, h : h + 1])
        key = (1.0 - low) * jax.nn.sigmoid(-forget)
        decay = jnp.where(live, decay, 1.0).reshape(group, new, width)
        key = jnp.where(live, key, 0.0).reshape(group, new, width)
        query = query.reshape(group, new, width)
        value3 = value.reshape(group, new, width)
        decayed = jnp.where(slot == 0, key, 0.0)
        total = decay[:, 0:1, :]
        carried = jnp.zeros_like(query)
        intra = jnp.zeros_like(query)
        for p in range(new):
            if p > 0:
                now = decay[:, p : p + 1, :]
                decayed = jnp.where(slot == p, key, decayed * now)
                total = total * now
            asked = query[:, p : p + 1, :]
            score = jnp.sum(asked * decayed, axis=2, keepdims=True)
            found = jnp.sum(score * value3, axis=1, keepdims=True)
            intra = jnp.where(slot == p, found, intra)
            carried = jnp.where(slot == p, asked * total, carried)
        stacked = jnp.concatenate(
            [
                decayed.reshape(lines, width),
                total.reshape(group, width),
                jnp.zeros((width - lines - group, width), F32),
            ],
            axis=0,
        )
        turned = stacked.T
        keys = turned[:, :lines].astype(BF16)
        reads = []
        for g in range(group):
            state = s_ref[0, g, h]
            reads.append(
                jnp.dot(
                    carried[g].astype(BF16), state.astype(BF16), preferred_element_type=F32
                )
            )
            mine = jnp.where(row // new == g, value, 0.0).astype(BF16)
            added = jnp.dot(keys, mine, preferred_element_type=F32)
            ns_ref[0, g, h] = turned[:, lines + g : lines + g + 1] * state + added
        read = jnp.concatenate(reads, axis=0) + intra.reshape(lines, width)
        scale = lax.rsqrt(jnp.mean(read * read, axis=1, keepdims=True) + EPSILON)
        out = read * scale * gain_ref[layer : layer + 1, cols] * (gate * jax.nn.sigmoid(gate))
        ho_ref[:, cols] = jnp.where(live, out, 0.0).astype(BF16)


def recurrence_call(layer, z, ext, low, gain, states, previous):
    blocks, seqs, heads, width, _ = states.shape
    new = z.shape[0] // seqs
    chans = heads * width
    lines = GROUP * new
    state_spec = pl.BlockSpec((1, GROUP, heads, width, width), lambda i: (layer, i, 0, 0, 0))
    in_specs = [
        pl.BlockSpec((lines, 4 * chans), lambda i: (i, 0)),
        pl.BlockSpec((lines, heads + 1), lambda i: (i, 0)),
        pl.BlockSpec((blocks, chans), lambda i: (0, 0)),
        pl.BlockSpec((blocks, chans), lambda i: (0, 0)),
        state_spec,
    ]
    args = [z, ext, low, gain, states]
    aliases = {}
    if previous is not None:
        in_specs.append(pl.BlockSpec(memory_space=pl.ANY))
        args.append(previous)
        aliases = {5: 1}
    return pl.pallas_call(
        functools.partial(recurrence_kernel, layer, heads, new),
        grid=(seqs // GROUP,),
        out_shape=[
            jax.ShapeDtypeStruct((z.shape[0], chans), BF16),
            jax.ShapeDtypeStruct(states.shape, F32),
        ],
        in_specs=in_specs,
        out_specs=[pl.BlockSpec((lines, chans), lambda i: (i, 0)), state_spec],
        input_output_aliases=aliases,
        compiler_params=pltpu.CompilerParams(
            dimension_semantics=("arbitrary",), vmem_limit_bytes=40 * 1024 * 1024
        ),
        name=f"recurrence{layer}",
    )(*args)


def local(
    activation_rows,
    fresh_spans,
    entry_rescale_vector,
    probe_kernel,
    retention_kernel,
    content_kernel,
    valve_kernel,
    retention_minimum,
    extra_attenuation,
    channel_rescale_vector,
    emission_kernel,
    memory_grids,
):
    n, t = lax.axis_size("dp"), lax.axis_size("tp")
    rows, feats = activation_rows.shape
    chans = probe_kernel.shape[2]
    own_seqs = fresh_spans.shape[0]
    seqs = own_seqs * n
    new = rows // seqs
    sizes = (n, t, rows, LIVE_PER_SEQUENCE * seqs, feats, chans)
    weights = (probe_kernel, retention_kernel, content_kernel, valve_kernel)

    spans = lax.all_gather(fresh_spans, "dp", axis=0, tiled=True)
    before = lax.broadcasted_iota(jnp.int32, (seqs, seqs), 1) < lax.broadcasted_iota(
        jnp.int32, (seqs, seqs), 0
    )
    starts = jnp.sum(jnp.where(before, spans[None, :], 0), axis=1)
    slots = lax.broadcasted_iota(jnp.int32, (seqs, new), 1)
    position = jnp.where(slots < spans[:, None], starts[:, None] + slots, -1).reshape(rows)
    posrow, poscol = position[None, :], position[:, None]
    own_live = (
        lax.broadcasted_iota(jnp.int32, (own_seqs, new), 1) < fresh_spans[:, None]
    ).reshape(own_seqs * new, 1)
    ext = [
        jnp.concatenate([extra_attenuation[b], own_live.astype(F32)], axis=1) for b in range(2)
    ]

    z, xc = comm_call(
        sizes, False, 0, 0, (posrow, activation_rows, poscol, entry_rescale_vector, *weights)
    )
    heads_out, states = recurrence_call(
        0, z, ext[0], retention_minimum, channel_rescale_vector, memory_grids, None
    )
    z, xc = comm_call(
        sizes, True, 1, 1,
        (posrow, heads_out, xc, emission_kernel, poscol, entry_rescale_vector, *weights),
    )
    heads_out, states = recurrence_call(
        1, z, ext[1], retention_minimum, channel_rescale_vector, memory_grids, states
    )
    (xc,) = comm_call(sizes, True, None, 2, (posrow, heads_out, xc, emission_kernel))
    spread = (
        lax.broadcasted_iota(jnp.int32, (rows, sizes[3]), 1) == poscol
    ).astype(BF16)
    moved = jnp.dot(spread, xc, preferred_element_type=F32).astype(BF16)
    mixed = jnp.where(poscol >= 0, moved, activation_rows)
    return (mixed, states)


def solution(mesh):
    placed = (
        P(None, "dp"),
        P("dp"),
        P(None, "dp"),
        P(None, "dp", "tp"),
        P(None, "dp", "tp"),
        P(None, "dp", "tp"),
        P(None, "dp", "tp"),
        P(None, "tp"),
        P(None, "dp", "tp"),
        P(None, "tp"),
        P(None, "tp", "dp"),
        P(None, "dp", "tp", None, None),
    )
    return jax.shard_map(
        local,
        mesh=mesh,
        in_specs=placed,
        out_specs=(P(None, "dp"), P(None, "dp", "tp", None, None)),
        check_vma=False,
    )
```
